32 devices in a mesh: sp: 4 (over z), tp: 4 (over y, x), dp: 2 (over core).
Axes of the slice: x: 2, y: 2, z: 4, core: 2. Of those that a mesh axis runs over, the one named last changes fastest.
Arguments:
- latent_tokens: bfloat16 [4096, 2048], P(('dp', 'sp', 'tp')), parts along dimension 0, may hold values from -6 to 6
- condition: bfloat16 [4096], P(('dp', 'sp')), parts along dimension 0, may hold values from -6 to 6
- shift_weight: bfloat16 [2048, 2048], P('sp', 'tp'), may hold values from -0.125 to 0.125
- scale_weight: bfloat16 [2048, 2048], P('sp', 'tp'), may hold values from -0.125 to 0.125
- gate_weight: bfloat16 [2048, 2048], P('sp', 'tp'), may hold values from -0.125 to 0.125
- norm_gain: float32 [2048], replicated, may hold values from 0.1 to 1.9
- query_down: bfloat16 [2048, 512], replicated, may hold values from -0.125 to 0.125
- query_gain: float32 [512], replicated, may hold values from 0.1 to 1.9
- kv_down: bfloat16 [2048, 256], replicated, may hold values from -0.125 to 0.125
- kv_gain: float32 [256], replicated, may hold values from 0.1 to 1.9
- rope_down: bfloat16 [2048, 32], replicated, may hold values from -0.125 to 0.125
- query_up: bfloat16 [512, 1536], P(None, 'tp'), may hold values from -0.25 to 0.25
- key_up: bfloat16 [256, 1024], P(None, 'tp'), may hold values from -0.375 to 0.375
- value_up: bfloat16 [256, 1024], P(None, 'tp'), may hold values from -0.375 to 0.375
- query_norm_gain: float32 [96], replicated, may hold values from 0.47 to 16
- key_norm_gain: float32 [96], replicated, may hold values from 0.47 to 16
- out_weight: bfloat16 [1024, 2048], P('tp'), may hold values from -0.1875 to 0.1875
- context_latent: bfloat16 [2048, 256], P(('dp', 'sp')), parts along dimension 0, may hold values from -6 to 6
- context_rope: bfloat16 [2048, 32], P(('dp', 'sp')), parts along dimension 0, may hold values from -6 to 6
- context_lift: float32 [16], P('tp'), may hold values from 0 to 2
Outputs:
- output: bfloat16 [4096, 2048], P(('dp', 'sp', 'tp')), parts along dimension 0
The draws below stay inside these ranges and needn't reach their ends.
There are 2 independent parts, one for each index of `dp`. The reference program is written for one: setup_inputs(seed, part) draws one part's arguments, and reference() takes and returns one part's arrays. A program takes and returns all parts, laid end to end along the dimension named above; an argument that names none is the same for every part. Nothing has to cross between parts.
All inputs are finite; a program needn't handle non-finite values.
Results may differ from the reference program's by a relative error of at most 0.015.
The reference program's roundings to bfloat16 on the way count: a program that leaves them out, or rounds other values in their place, can miss the bound.
Values may be sent and summed in bfloat16 or wider, within the bound.
No kernel may reach another device: no remote copies, remote signals or barrier semaphores. Data moves between devices by JAX's collectives and lax.ppermute only.
A program may use at most 128 MiB of HBM per device.

```python
import jax
import jax.numpy as jnp
from jax import lax

D_MODEL = 2048
HEADS = 16
NOPE_DIM = 64
ROPE_DIM = 32
VALUE_DIM = 64
QK_DIM = 96
Q_RANK = 512
KV_RANK = 256
GRID_W = 64
CONTEXT = 1024
TOKENS = 2048
N_TP = 4


def gain_draw(key, salt):
    own_key = jax.random.fold_in(key, salt)
    normal_values = jax.random.normal(own_key, (QK_DIM,), jnp.float32)
    return 1.7 * (1.0 + 0.18 * jnp.clip(normal_values, -4.0, 4.0))


def draw_query_norm_gain(key, part):
    return gain_draw(key, 31)


def draw_key_norm_gain(key, part):
    return gain_draw(key, 57)


def block_scale(rng, dims, cuts, least, top_value):
    loudness = 1.0
    for dim, shards_of in cuts:
        heights = jax.random.uniform(jax.random.fold_in(jax.random.fold_in(rng, 6), dim), (shards_of,), jnp.float32, least / len(cuts), top_value / len(cuts))
        loudness = loudness * jnp.repeat(jnp.exp(heights), dims[dim] // shards_of).reshape((-1,) + (1,) * (len(dims) - 1 - dim))
    return loudness


def bell_draw(key, shape, spread, bound, shards=(), kind=jnp.bfloat16):
    drawn = spread * jax.random.normal(key, shape, jnp.float32)
    if shards:
        drawn = drawn * block_scale(key, shape, shards, -0.22, 0.18)
    return jnp.clip(drawn, -bound, bound).astype(kind)


def setup_inputs(seed: int = 0, part: int = 0) -> dict:
    key_of = jax.random.split(jax.random.key(seed), 21)
    part_keys = jax.random.split(jax.random.fold_in(key_of[20], part), 21)
    latent_tokens = bell_draw(part_keys[0], (TOKENS, D_MODEL), 1.0, 6.0, ((0, 16),))
    condition = bell_draw(part_keys[1], (D_MODEL,), 1.0, 6.0, ((0, 4),))
    shift_weight = bell_draw(key_of[2], (D_MODEL, D_MODEL), D_MODEL ** -0.5, 0.125, ((0, 4), (1, 4)))
    scale_weight = bell_draw(key_of[3], (D_MODEL, D_MODEL), D_MODEL ** -0.5, 0.125, ((0, 4), (1, 4)))
    gate_weight = bell_draw(key_of[4], (D_MODEL, D_MODEL), D_MODEL ** -0.5, 0.125, ((0, 4), (1, 4)))
    norm_gain = jnp.clip(1.0 + 0.18 * jax.random.normal(key_of[5], (D_MODEL,), jnp.float32), 0.1, 1.9)
    query_down = bell_draw(key_of[6], (D_MODEL, Q_RANK), D_MODEL ** -0.5, 0.125)
    query_gain = jnp.clip(1.0 + 0.18 * jax.random.normal(key_of[7], (Q_RANK,), jnp.float32), 0.1, 1.9)
    kv_down = bell_draw(key_of[8], (D_MODEL, KV_RANK), D_MODEL ** -0.5, 0.125)
    kv_gain = jnp.clip(1.0 + 0.18 * jax.random.normal(key_of[9], (KV_RANK,), jnp.float32), 0.1, 1.9)
    rope_down = bell_draw(key_of[10], (D_MODEL, ROPE_DIM), D_MODEL ** -0.5, 0.125)
    query_up = bell_draw(key_of[11], (Q_RANK, HEADS * QK_DIM), Q_RANK ** -0.5, 0.25, ((1, 4),))
    key_up = bell_draw(key_of[12], (KV_RANK, HEADS * NOPE_DIM), KV_RANK ** -0.5, 0.375, ((1, 4),))
    value_up = bell_draw(key_of[13], (KV_RANK, HEADS * VALUE_DIM), KV_RANK ** -0.5, 0.375, ((1, 4),))
    query_norm_gain = draw_query_norm_gain(jax.random.fold_in(key_of[20], 71), part)
    key_norm_gain = draw_key_norm_gain(jax.random.fold_in(key_of[20], 71), part)
    out_weight = bell_draw(key_of[16], (HEADS * VALUE_DIM, D_MODEL), (HEADS * VALUE_DIM) ** -0.5, 0.1875, ((0, 4),))
    context_latent = bell_draw(part_keys[17], (CONTEXT, KV_RANK), 1.0, 6.0, ((0, 4),))
    context_rope = bell_draw(part_keys[18], (CONTEXT, ROPE_DIM), 1.0, 6.0, ((0, 4),))
    context_lift = jnp.clip(2.0 * jax.random.uniform(key_of[19], (HEADS,), jnp.float32) ** block_scale(key_of[19], (HEADS,), ((0, 4),), -0.2, 0.2), 0.0, 2.0)
    return {"latent_tokens": latent_tokens, "condition": condition, "shift_weight": shift_weight, "scale_weight": scale_weight, "gate_weight": gate_weight, "norm_gain": norm_gain, "query_down": query_down, "query_gain": query_gain, "kv_down": kv_down, "kv_gain": kv_gain, "rope_down": rope_down, "query_up": query_up, "key_up": key_up, "value_up": value_up, "query_norm_gain": query_norm_gain, "key_norm_gain": key_norm_gain, "out_weight": out_weight, "context_latent": context_latent, "context_rope": context_rope, "context_lift": context_lift}


EPS = 1e-06
THETA = 10000.0

def rms_scaled(values, gain_vector):
    mean_square = lax.optimization_barrier(jnp.mean(values * values, axis=-1, keepdims=True))
    return values * lax.rsqrt(mean_square + EPS) * gain_vector

def rotate(rope_part, positions):
    row_count = rope_part.shape[0]
    freq_count = ROPE_DIM // 4
    inverse = THETA ** (-4.0 * jnp.arange(freq_count, dtype=jnp.float32) / ROPE_DIM)
    grid_row = (positions // GRID_W).astype(jnp.float32)
    grid_col = (positions % GRID_W).astype(jnp.float32)
    angles = jnp.stack([grid_row[:, None] * inverse, grid_col[:, None] * inverse], axis=1)
    cosine_table = jnp.cos(angles)[:, None]
    sine_table = jnp.sin(angles)[:, None]
    split_rows = rope_part.reshape(row_count, rope_part.shape[1], 2, 2, freq_count)
    first_half = split_rows[:, :, :, 0]
    second_half = split_rows[:, :, :, 1]
    turned = jnp.stack([first_half * cosine_table - second_half * sine_table, second_half * cosine_table + first_half * sine_table], axis=3)
    return turned.reshape(rope_part.shape)

def expand(latent_rows, rope_rows, key_up, value_up, key_norm_gain):
    row_count = latent_rows.shape[0]
    nope_part = jnp.dot(latent_rows, key_up, preferred_element_type=jnp.float32).reshape(row_count, HEADS, NOPE_DIM)
    value_rows = jnp.dot(latent_rows, value_up, preferred_element_type=jnp.float32).astype(jnp.bfloat16)
    shared = jnp.broadcast_to(rope_rows.astype(jnp.float32)[:, None, :], (row_count, HEADS, ROPE_DIM))
    normal_keys = rms_scaled(jnp.concatenate([nope_part, shared], axis=-1), key_norm_gain)
    return (normal_keys, value_rows.reshape(row_count, HEADS, VALUE_DIM))

def reference(latent_tokens, condition, shift_weight, scale_weight, gate_weight, norm_gain, query_down, query_gain, kv_down, kv_gain, rope_down, query_up, key_up, value_up, query_norm_gain, key_norm_gain, out_weight, context_latent, context_rope, context_lift):
    activated = jax.nn.silu(condition.astype(jnp.float32)).astype(jnp.bfloat16)[None]
    mod_shift = jnp.dot(activated, shift_weight, preferred_element_type=jnp.float32)[0]
    mod_scale = jnp.dot(activated, scale_weight, preferred_element_type=jnp.float32)[0]
    mod_gate = jnp.dot(activated, gate_weight, preferred_element_type=jnp.float32)[0]
    token_values = latent_tokens.astype(jnp.float32)
    normed = (rms_scaled(token_values, norm_gain) * (1.0 + mod_scale) + mod_shift).astype(jnp.bfloat16)
    query_latent = rms_scaled(jnp.dot(normed, query_down, preferred_element_type=jnp.float32), query_gain).astype(jnp.bfloat16)
    key_latent = rms_scaled(jnp.dot(normed, kv_down, preferred_element_type=jnp.float32), kv_gain).astype(jnp.bfloat16)
    rope_key = jnp.dot(normed, rope_down, preferred_element_type=jnp.float32).astype(jnp.bfloat16)
    positions = jnp.arange(TOKENS, dtype=jnp.int32)
    query_heads = rms_scaled(jnp.dot(query_latent, query_up, preferred_element_type=jnp.float32).reshape(TOKENS, HEADS, QK_DIM), query_norm_gain)
    queries = jnp.concatenate([query_heads[..., :NOPE_DIM], rotate(query_heads[..., NOPE_DIM:], positions)], axis=-1).astype(jnp.bfloat16)
    latent_normal, latent_values = expand(key_latent, rope_key, key_up, value_up, key_norm_gain)
    latent_keys = jnp.concatenate([latent_normal[..., :NOPE_DIM], rotate(latent_normal[..., NOPE_DIM:], positions)], axis=-1).astype(jnp.bfloat16)
    context_normal, context_values = expand(context_latent, context_rope, key_up, value_up, key_norm_gain)
    context_keys = context_normal.astype(jnp.bfloat16)
    all_keys = jnp.concatenate([latent_keys, context_keys], axis=0)
    all_values = jnp.concatenate([latent_values, context_values], axis=0)
    is_context = jnp.arange(TOKENS + CONTEXT, dtype=jnp.int32) >= TOKENS

    def one_head(inputs):
        query_head, key_head, value_head, lift_head = inputs
        scores = jnp.dot(query_head, key_head.T, preferred_element_type=jnp.float32) * QK_DIM ** (-0.5)
        scores = scores + jnp.where(is_context, lift_head, jnp.zeros((), jnp.float32))[None, :]
        top_score = lax.optimization_barrier(jnp.max(scores, axis=-1, keepdims=True))
        weights = jnp.exp(scores - top_score)
        weight_total = lax.optimization_barrier(jnp.sum(weights, axis=-1, keepdims=True))
        summed = jnp.dot(weights.astype(jnp.bfloat16), value_head, preferred_element_type=jnp.float32)
        return (summed / weight_total).astype(jnp.bfloat16)
    attended = lax.map(one_head, (jnp.transpose(queries, (1, 0, 2)), jnp.transpose(all_keys, (1, 0, 2)), jnp.transpose(all_values, (1, 0, 2)), context_lift))
    attended = jnp.transpose(attended, (1, 0, 2)).reshape(TOKENS, HEADS * VALUE_DIM)
    group_width = HEADS // N_TP * VALUE_DIM
    mixed_sum = jnp.zeros((TOKENS, D_MODEL), jnp.float32)
    for head_group in range(N_TP):
        group_term = jnp.dot(attended[:, head_group * group_width:(head_group + 1) * group_width], out_weight[head_group * group_width:(head_group + 1) * group_width], preferred_element_type=jnp.float32)
        rounded = lax.optimization_barrier(group_term.astype(jnp.bfloat16))
        mixed_sum = mixed_sum + rounded.astype(jnp.float32)
    return (token_values + mod_gate * mixed_sum).astype(jnp.bfloat16)
```

```python
import functools
import math

import jax
import jax.numpy as jnp
import numpy as np
from jax import lax
from jax.experimental import pallas as pl
from jax.experimental.pallas import tpu as pltpu
from jax.sharding import PartitionSpec as P

NOPE_DIM = 64
ROPE_DIM = 32
VALUE_DIM = 64
QK_DIM = 96
PAD_DIM = 128
GRID_W = 64

EPS = 1e-06
THETA = 10000.0

F32 = jnp.float32
BF16 = jnp.bfloat16


def rms_scaled(values, gain_vector):
    mean_square = jnp.mean(values * values, axis=-1, keepdims=True)
    return values * lax.rsqrt(mean_square + EPS) * gain_vector


def turn_tables(token_count):
    freq_count = ROPE_DIM // 4
    inverse = (THETA ** (-4.0 * np.arange(freq_count) / ROPE_DIM)).astype(np.float32)
    index = np.arange(token_count)
    row = (index // GRID_W).astype(np.float32)
    col = (index % GRID_W).astype(np.float32)
    angles = np.concatenate([inverse[:, None] * row, inverse[:, None] * col], axis=0)
    angles = angles.astype(np.float64)
    return np.cos(angles).astype(np.float32), np.sin(angles).astype(np.float32)


def turn(part, cosine, sine):
    f = ROPE_DIM // 4
    u0, w0, u1, w1 = part[:f], part[f : 2 * f], part[2 * f : 3 * f], part[3 * f :]
    c0, c1, s0, s1 = cosine[:f], cosine[f:], sine[:f], sine[f:]
    return jnp.concatenate(
        [u0 * c0 - w0 * s0, w0 * c0 + u0 * s0, u1 * c1 - w1 * s1, w1 * c1 + u1 * s1], axis=0
    )


def contract(a, b, dims):
    return lax.dot_general(a, b, (dims, ((), ())), preferred_element_type=F32)


def attention_kernel(
    query_ref,
    latent_ref,
    context_ref,
    query_up_ref,
    key_up_ref,
    value_up_ref,
    query_gain_ref,
    key_gain_ref,
    lift_ref,
    cos_query_ref,
    sin_query_ref,
    cos_key_ref,
    sin_key_ref,
    out_ref,
    keys,
    values,
    queries,
    scores,
    *,
    head_count,
    chunk,
    row_block,
):
    rank = key_up_ref.shape[0]
    latent_count = latent_ref.shape[0]
    context_count = context_ref.shape[0]
    key_count = latent_count + context_count
    row_count = query_ref.shape[0]
    key_gain = key_gain_ref[...]
    query_gain = query_gain_ref[...]
    eye = (
        lax.broadcasted_iota(jnp.int32, (ROPE_DIM, ROPE_DIM), 0)
        == lax.broadcasted_iota(jnp.int32, (ROPE_DIM, ROPE_DIM), 1)
    ).astype(BF16)

    def build(rows, target, width, tables, is_context):
        latent = rows[:, :rank]
        nope = contract(key_up_ref[...], latent, ((0,), (1,)))
        rope = contract(eye, rows[:, rank : rank + ROPE_DIM], ((1,), (1,)))
        rope_square = jnp.sum(rope * rope, axis=0, keepdims=True)
        rope = rope * key_gain[NOPE_DIM:]
        if tables is not None:
            rope = turn(rope, *tables)
        for head in range(head_count):
            part = nope[head * NOPE_DIM : (head + 1) * NOPE_DIM]
            square = jnp.sum(part * part, axis=0, keepdims=True) + rope_square
            inverse = lax.rsqrt(square * (1.0 / QK_DIM) + EPS)
            if is_context:
                lift = jnp.full((16, width), lift_ref[0, head] * math.sqrt(QK_DIM), F32)
                high = lift.astype(BF16).astype(F32)
                middle = (lift - high).astype(BF16).astype(F32)
                low = lift - high - middle
                index = lax.broadcasted_iota(jnp.int32, (16, width), 0)
                extra = jnp.where(
                    index == 0,
                    high,
                    jnp.where(index == 1, middle, jnp.where(index == 2, low, 0.0)),
                )
            else:
                extra = jnp.zeros((16, width), F32)
            keys[head, :, target] = jnp.concatenate(
                [
                    part * key_gain[:NOPE_DIM] * inverse,
                    rope * inverse,
                    extra,
                    jnp.zeros((16, width), F32),
                ],
                axis=0,
            ).astype(BF16)
        value = jnp.dot(latent, value_up_ref[...], preferred_element_type=F32)
        lane = lax.broadcasted_iota(jnp.int32, (width, PAD_DIM), 1)
        for pair in range(head_count // 2):
            both = value[:, pair * PAD_DIM : (pair + 1) * PAD_DIM]
            one_even = (lane == VALUE_DIM).astype(F32)
            one_odd = (lane == 0).astype(F32)
            values[2 * pair, target, :] = jnp.where(lane < VALUE_DIM, both, one_even).astype(BF16)
            values[2 * pair + 1, target, :] = jnp.where(
                lane >= VALUE_DIM, both, one_odd
            ).astype(BF16)

    def latent_chunk(i, carry):
        at = pl.ds(pl.multiple_of(i * chunk, chunk), chunk)
        build(latent_ref[at, :], at, chunk, (cos_key_ref[:, at], sin_key_ref[:, at]), False)
        return carry

    lax.fori_loop(0, latent_count // chunk, latent_chunk, 0)

    def context_chunk(i, carry):
        source = pl.ds(pl.multiple_of(i * chunk, chunk), chunk)
        target = pl.ds(pl.multiple_of(latent_count + i * chunk, chunk), chunk)
        build(context_ref[source, :], target, chunk, None, True)
        return carry

    lax.fori_loop(0, context_count // chunk, context_chunk, 0)

    projected = contract(query_up_ref[...], query_ref[...], ((0,), (1,)))
    for head in range(head_count):
        part = projected[head * QK_DIM : (head + 1) * QK_DIM]
        inverse = lax.rsqrt(jnp.mean(part * part, axis=0, keepdims=True) + EPS)
        part = part * inverse * query_gain
        turned = turn(part[NOPE_DIM:], cos_query_ref[...], sin_query_ref[...])
        extra = (
            lax.broadcasted_iota(jnp.int32, (PAD_DIM - QK_DIM, row_count), 0) < 3
        ).astype(F32)
        whole = jnp.concatenate([part[:NOPE_DIM], turned, extra], axis=0)
        queries[head] = whole.T.astype(BF16)

    scale = QK_DIM**-0.5 * math.log2(math.e)
    chunks = key_count // chunk
    blocks = row_count // row_block

    def score_chunk(slot, head, rows, index, top):
        at = slice(index * chunk, (index + 1) * chunk)
        part = jnp.dot(queries[head, rows, :], keys[head, :, at], preferred_element_type=F32)
        scores[slot, :, at] = part
        for start in range(0, chunk, PAD_DIM):
            piece = part[:, start : start + PAD_DIM]
            top = piece if top is None else jnp.maximum(top, piece)
        return top

    def weigh_chunk(slot, head, index, top, total):
        at = slice(index * chunk, (index + 1) * chunk)
        weights = jnp.exp2((scores[slot, :, at] - top) * scale).astype(BF16)
        product = jnp.dot(weights, values[head, at, :], preferred_element_type=F32)
        return product if total is None else total + product

    def both_steps(slot, head, top, next_head, next_rows):
        top = jnp.max(top, axis=1, keepdims=True)
        next_top = None
        total = None
        for index in range(chunks):
            next_top = score_chunk(1 - slot, next_head, next_rows, index, next_top)
            total = weigh_chunk(slot, head, index, top, total)
        return total, next_top

    first = None
    for index in range(chunks):
        first = score_chunk(0, 0, slice(0, row_block), index, first)

    lane = lax.broadcasted_iota(jnp.int32, (row_block, PAD_DIM), 1)

    def pair_step(pair, top):
        even, odd = 2 * pair, 2 * pair + 1
        following = jnp.minimum(even + 2, head_count - 2)
        for block in range(blocks):
            rows = slice(block * row_block, (block + 1) * row_block)
            even_total, top = both_steps(0, even, top, odd, rows)
            if block + 1 < blocks:
                next_head = even
                next_rows = slice((block + 1) * row_block, (block + 2) * row_block)
            else:
                next_head = following
                next_rows = slice(0, row_block)
            odd_total, top = both_steps(1, odd, top, next_head, next_rows)
            joined = jnp.where(
                lane < VALUE_DIM,
                even_total / even_total[:, VALUE_DIM : VALUE_DIM + 1],
                odd_total / odd_total[:, 0:1],
            )
            out_ref[rows, pl.ds(pl.multiple_of(pair * PAD_DIM, PAD_DIM), PAD_DIM)] = joined.astype(
                BF16
            )
        return top

    lax.fori_loop(0, head_count // 2, pair_step, first)


def attend(query, latent, context, query_up, key_up, value_up, gains, lift, tables):
    row_count = query.shape[0]
    key_count = latent.shape[0] + context.shape[0]
    head_count = query_up.shape[1] // QK_DIM
    row_block = min(256, row_count)
    vmem = pl.BlockSpec(memory_space=pltpu.VMEM)
    return pl.pallas_call(
        functools.partial(
            attention_kernel, head_count=head_count, chunk=512, row_block=row_block
        ),
        out_shape=jax.ShapeDtypeStruct((row_count, head_count * VALUE_DIM), BF16),
        in_specs=[vmem] * 8 + [pl.BlockSpec(memory_space=pltpu.SMEM)] + [vmem] * 4,
        out_specs=vmem,
        scratch_shapes=[
            pltpu.VMEM((head_count, PAD_DIM, key_count), BF16),
            pltpu.VMEM((head_count, key_count, PAD_DIM), BF16),
            pltpu.VMEM((head_count, row_count, PAD_DIM), BF16),
            pltpu.VMEM((2, row_block, key_count), F32),
        ],
        compiler_params=pltpu.CompilerParams(vmem_limit_bytes=60 * 1024 * 1024),
        name="attend",
    )(query, latent, context, query_up, key_up, value_up, *gains, lift, *tables)


def project_kernel(attended_ref, weight_ref, token_ref, gate_ref, out_ref):
    groups = weight_ref.shape[0]
    mixed = None
    for group in range(groups):
        term = jnp.dot(attended_ref[group], weight_ref[group], preferred_element_type=F32)
        term = term.astype(BF16).astype(F32)
        mixed = term if mixed is None else mixed + term
    out_ref[...] = (token_ref[...].astype(F32) + gate_ref[...] * mixed).astype(BF16)


def project(attended, weight, tokens, gate):
    groups, rows, width = attended.shape
    model = tokens.shape[1]
    block = min(512, model)
    return pl.pallas_call(
        project_kernel,
        grid=(model // block,),
        out_shape=jax.ShapeDtypeStruct(tokens.shape, BF16),
        in_specs=[
            pl.BlockSpec((groups, rows, width), lambda i: (0, 0, 0)),
            pl.BlockSpec((groups, width, block), lambda i: (0, 0, i)),
            pl.BlockSpec((rows, block), lambda i: (0, i)),
            pl.BlockSpec((1, block), lambda i: (0, i)),
        ],
        out_specs=pl.BlockSpec((rows, block), lambda i: (0, i)),
        name="project",
    )(attended, weight, tokens, gate)


def spread(block, axes, count):
    copies = jnp.broadcast_to(block[None], (count,) + block.shape)
    return lax.all_to_all(copies, axes, 0, 0)


def local(
    n_sp,
    n_tp,
    latent_tokens,
    condition,
    shift_weight,
    scale_weight,
    gate_weight,
    norm_gain,
    query_down,
    query_gain,
    kv_down,
    kv_gain,
    rope_down,
    query_up,
    key_up,
    value_up,
    query_norm_gain,
    key_norm_gain,
    out_weight,
    context_latent,
    context_rope,
    context_lift,
):
    model = latent_tokens.shape[1]
    activated = jax.nn.silu(condition.astype(F32)).astype(BF16)[None]
    terms = jnp.concatenate(
        [
            jnp.dot(activated, weight, preferred_element_type=F32)
            for weight in (shift_weight, scale_weight, gate_weight)
        ],
        axis=0,
    )
    gathered = spread(terms, ("sp", "tp"), n_sp * n_tp)
    context = spread(
        jnp.concatenate([context_latent, context_rope], axis=1), "sp", n_sp
    ).reshape(-1, context_latent.shape[1] + context_rope.shape[1])
    all_weight = spread(out_weight, "tp", n_tp)
    summed = jnp.sum(gathered.reshape(n_sp, n_tp, 3, -1), axis=0)
    mod = jnp.transpose(summed, (1, 0, 2)).reshape(3, model)
    token_values = latent_tokens.astype(F32)
    normed = (rms_scaled(token_values, norm_gain) * (1.0 + mod[1]) + mod[0]).astype(BF16)
    key_latent = rms_scaled(
        jnp.dot(normed, kv_down, preferred_element_type=F32), kv_gain
    ).astype(BF16)
    rope_key = jnp.dot(normed, rope_down, preferred_element_type=F32).astype(BF16)
    latent = spread(
        jnp.concatenate([key_latent, rope_key], axis=1), ("sp", "tp"), n_sp * n_tp
    ).reshape(-1, context.shape[1])
    query_latent = rms_scaled(
        jnp.dot(normed, query_down, preferred_element_type=F32), query_gain
    ).astype(BF16)
    query_group = spread(query_latent, "tp", n_tp).reshape(-1, query_latent.shape[1])
    group_rows = query_group.shape[0]
    cosine, sine = (jnp.asarray(t) for t in turn_tables(latent.shape[0]))
    start = lax.axis_index("sp") * group_rows
    own = [lax.dynamic_slice_in_dim(t, start, group_rows, 1) for t in (cosine, sine)]
    attended = attend(
        query_group,
        latent,
        context,
        query_up,
        key_up,
        value_up,
        (query_norm_gain[:, None], key_norm_gain[:, None]),
        context_lift[None],
        (*own, cosine, sine),
    )
    shared = lax.all_to_all(
        attended.reshape(n_tp, group_rows // n_tp, attended.shape[1]), "tp", 0, 0
    )
    return project(shared, all_weight, latent_tokens, mod[2:3])


def solution(mesh):
    in_specs = (
        P(("dp", "sp", "tp"), None),
        P(("dp", "sp")),
        P("sp", "tp"),
        P("sp", "tp"),
        P("sp", "tp"),
        P(),
        P(),
        P(),
        P(),
        P(),
        P(),
        P(None, "tp"),
        P(None, "tp"),
        P(None, "tp"),
        P(),
        P(),
        P("tp", None),
        P(("dp", "sp"), None),
        P(("dp", "sp"), None),
        P("tp"),
    )
    out_specs = P(("dp", "sp", "tp"), None)
    body = functools.partial(local, mesh.shape["sp"], mesh.shape["tp"])
    return jax.shard_map(body, mesh=mesh, in_specs=in_specs, out_specs=out_specs, check_vma=False)
```

```python
import functools
import math

import jax
import jax.numpy as jnp
import numpy as np
from jax import lax
from jax.experimental import pallas as pl
from jax.experimental.pallas import tpu as pltpu
from jax.sharding import PartitionSpec as P

NOPE_DIM = 64
ROPE_DIM = 32
VALUE_DIM = 64
QK_DIM = 96
PAD_DIM = 128
GRID_W = 64

EPS = 1e-06
THETA = 10000.0


F32 = jnp.float32
BF16 = jnp.bfloat16


def rms_scaled(values, gain_vector):
    mean_square = jnp.mean(values * values, axis=-1, keepdims=True)
    return values * lax.rsqrt(mean_square + EPS) * gain_vector


def turn_tables(token_count):
    freq_count = ROPE_DIM // 4
    inverse = (THETA ** (-4.0 * np.arange(freq_count) / ROPE_DIM)).astype(np.float32)
    index = np.arange(token_count)
    row = (index // GRID_W).astype(np.float32)
    col = (index % GRID_W).astype(np.float32)
    angles = np.concatenate([inverse[:, None] * row, inverse[:, None] * col], axis=0)
    angles = angles.astype(np.float64)
    return np.cos(angles).astype(np.float32), np.sin(angles).astype(np.float32)


def turn(part, cosine, sine):
    f = ROPE_DIM // 4
    u0, w0, u1, w1 = part[:f], part[f : 2 * f], part[2 * f : 3 * f], part[3 * f :]
    c0, c1, s0, s1 = cosine[:f], cosine[f:], sine[:f], sine[f:]
    return jnp.concatenate(
        [u0 * c0 - w0 * s0, w0 * c0 + u0 * s0, u1 * c1 - w1 * s1, w1 * c1 + u1 * s1], axis=0
    )


def contract(a, b, dims):
    return lax.dot_general(a, b, (dims, ((), ())), preferred_element_type=F32)


def attention_kernel(
    query_ref,
    latent_ref,
    context_ref,
    query_up_ref,
    key_up_ref,
    value_up_ref,
    query_gain_ref,
    key_gain_ref,
    lift_ref,
    cos_query_ref,
    sin_query_ref,
    cos_key_ref,
    sin_key_ref,
    out_ref,
    keys,
    values,
    queries,
    scores,
    *,
    head_count,
    chunk,
    row_block,
):
    rank = key_up_ref.shape[0]
    latent_block = latent_ref.shape[2]
    context_block = context_ref.shape[2]
    latent_count = latent_ref.shape[0] * latent_block
    context_count = context_ref.shape[0] * context_block
    key_count = latent_count + context_count
    row_count = query_ref.shape[0]
    key_gain = key_gain_ref[...]
    query_gain = query_gain_ref[...]
    def build(rows, target, width, tables, is_context):
        latent = rows[:rank]
        nope = contract(key_up_ref[...], latent, ((0,), (0,)))
        rope = rows[rank : rank + ROPE_DIM].astype(F32)
        rope_square = jnp.sum(rope * rope, axis=0, keepdims=True)
        rope = rope * key_gain[NOPE_DIM:]
        if tables is not None:
            rope = turn(rope, *tables)
        for head in range(head_count):
            part = nope[head * NOPE_DIM : (head + 1) * NOPE_DIM]
            square = jnp.sum(part * part, axis=0, keepdims=True) + rope_square
            inverse = lax.rsqrt(square * (1.0 / QK_DIM) + EPS)
            if is_context:
                lift = jnp.full((16, width), lift_ref[0, head] * math.sqrt(QK_DIM), F32)
                high = lift.astype(BF16).astype(F32)
                middle = (lift - high).astype(BF16).astype(F32)
                low = lift - high - middle
                index = lax.broadcasted_iota(jnp.int32, (16, width), 0)
                extra = jnp.where(
                    index == 0,
                    high,
                    jnp.where(index == 1, middle, jnp.where(index == 2, low, 0.0)),
                )
            else:
                extra = jnp.zeros((16, width), F32)
            keys[head, :, target] = jnp.concatenate(
                [
                    part * key_gain[:NOPE_DIM] * inverse,
                    rope * inverse,
                    extra,
                    jnp.zeros((16, width), F32),
                ],
                axis=0,
            ).astype(BF16)
        value = contract(latent, value_up_ref[...], ((0,), (0,)))
        lane = lax.broadcasted_iota(jnp.int32, (width, PAD_DIM), 1)
        for pair in range(head_count // 2):
            both = value[:, pair * PAD_DIM : (pair + 1) * PAD_DIM]
            one_even = (lane == VALUE_DIM).astype(F32)
            one_odd = (lane == 0).astype(F32)
            values[2 * pair, target, :] = jnp.where(lane < VALUE_DIM, both, one_even).astype(BF16)
            values[2 * pair + 1, target, :] = jnp.where(
                lane >= VALUE_DIM, both, one_odd
            ).astype(BF16)

    def gathered(ref, block, i):
        count = chunk // block
        return jnp.concatenate([ref[i * count + j] for j in range(count)], axis=1)

    def latent_chunk(i, carry):
        at = pl.ds(pl.multiple_of(i * chunk, chunk), chunk)
        build(gathered(latent_ref, latent_block, i), at, chunk, (cos_key_ref[:, at], sin_key_ref[:, at]), False)
        return carry

    lax.fori_loop(0, latent_count // chunk, latent_chunk, 0)

    def context_chunk(i, carry):
        target = pl.ds(pl.multiple_of(latent_count + i * chunk, chunk), chunk)
        build(gathered(context_ref, context_block, i), target, chunk, None, True)
        return carry

    lax.fori_loop(0, context_count // chunk, context_chunk, 0)

    projected = contract(query_up_ref[...], query_ref[...], ((0,), (1,)))
    for head in range(head_count):
        part = projected[head * QK_DIM : (head + 1) * QK_DIM]
        inverse = lax.rsqrt(jnp.mean(part * part, axis=0, keepdims=True) + EPS)
        part = part * inverse * query_gain
        turned = turn(part[NOPE_DIM:], cos_query_ref[...], sin_query_ref[...])
        extra = (
            lax.broadcasted_iota(jnp.int32, (PAD_DIM - QK_DIM, row_count), 0) < 3
        ).astype(F32)
        whole = jnp.concatenate([part[:NOPE_DIM], turned, extra], axis=0)
        queries[head] = whole.T.astype(BF16)

    scale = QK_DIM**-0.5 * math.log2(math.e)
    chunks = key_count // chunk
    blocks = row_count // row_block

    def score_chunk(slot, head, rows, index, top):
        at = slice(index * chunk, (index + 1) * chunk)
        part = jnp.dot(queries[head, rows, :], keys[head, :, at], preferred_element_type=F32)
        scores[slot, :, at] = part
        for start in range(0, chunk, PAD_DIM):
            piece = part[:, start : start + PAD_DIM]
            top = piece if top is None else jnp.maximum(top, piece)
        return top

    def weigh_chunk(slot, head, index, top, total):
        at = slice(index * chunk, (index + 1) * chunk)
        weights = jnp.exp2((scores[slot, :, at] - top) * scale).astype(BF16)
        product = jnp.dot(weights, values[head, at, :], preferred_element_type=F32)
        return product if total is None else total + product

    def both_steps(slot, head, top, next_head, next_rows):
        top = jnp.max(top, axis=1, keepdims=True)
        next_top = None
        total = None
        for index in range(chunks):
            next_top = score_chunk(1 - slot, next_head, next_rows, index, next_top)
            total = weigh_chunk(slot, head, index, top, total)
        return total, next_top

    first = None
    for index in range(chunks):
        first = score_chunk(0, 0, slice(0, row_block), index, first)

    lane = lax.broadcasted_iota(jnp.int32, (row_block, PAD_DIM), 1)

    def pair_step(pair, top):
        even, odd = 2 * pair, 2 * pair + 1
        following = jnp.minimum(even + 2, head_count - 2)
        for block in range(blocks):
            rows = slice(block * row_block, (block + 1) * row_block)
            even_total, top = both_steps(0, even, top, odd, rows)
            if block + 1 < blocks:
                next_head = even
                next_rows = slice((block + 1) * row_block, (block + 2) * row_block)
            else:
                next_head = following
                next_rows = slice(0, row_block)
            odd_total, top = both_steps(1, odd, top, next_head, next_rows)
            joined = jnp.where(
                lane < VALUE_DIM,
                even_total / even_total[:, VALUE_DIM : VALUE_DIM + 1],
                odd_total / odd_total[:, 0:1],
            )
            out_ref[rows, pl.ds(pl.multiple_of(pair * PAD_DIM, PAD_DIM), PAD_DIM)] = joined.astype(
                BF16
            )
        return top

    lax.fori_loop(0, head_count // 2, pair_step, first)


def attend(query, latent, context, query_up, key_up, value_up, gains, lift, tables):
    row_count = query.shape[0]
    key_count = latent.shape[0] * latent.shape[2] + context.shape[0] * context.shape[2]
    head_count = query_up.shape[1] // QK_DIM
    row_block = min(256, row_count)
    vmem = pl.BlockSpec(memory_space=pltpu.VMEM)
    return pl.pallas_call(
        functools.partial(
            attention_kernel, head_count=head_count, chunk=512, row_block=row_block
        ),
        out_shape=jax.ShapeDtypeStruct((row_count, head_count * VALUE_DIM), BF16),
        in_specs=[vmem] * 8 + [pl.BlockSpec(memory_space=pltpu.SMEM)] + [vmem] * 4,
        out_specs=vmem,
        scratch_shapes=[
            pltpu.VMEM((head_count, PAD_DIM, key_count), BF16),
            pltpu.VMEM((head_count, key_count, PAD_DIM), BF16),
            pltpu.VMEM((head_count, row_count, PAD_DIM), BF16),
            pltpu.VMEM((2, row_block, key_count), F32),
        ],
        compiler_params=pltpu.CompilerParams(vmem_limit_bytes=60 * 1024 * 1024),
        name="attend",
    )(query, latent, context, query_up, key_up, value_up, *gains, lift, *tables)


def project_kernel(place_ref, groups, *refs):
    attended, own_ref = refs[:groups], refs[groups]
    token_ref, gate_ref, out_ref = refs[-3:]
    parts = refs[groups + 1 : -3]
    for part, part_ref in enumerate(parts):

        @pl.when(pl.program_id(0) == part)
        def _():
            mixed = None
            for group in range(groups):
                weight = own_ref[...] if group == 0 else part_ref[group - 1]
                term = jnp.dot(attended[group][...], weight, preferred_element_type=F32)
                term = term.astype(BF16).astype(F32)
                mixed = term if mixed is None else mixed + term
            out_ref[...] = (token_ref[...].astype(F32) + gate_ref[...] * mixed).astype(BF16)


def project(place, attended, own_weight, parts, tokens, gate):
    groups = len(attended)
    rows, width = attended[0].shape
    model = tokens.shape[1]
    count = len(parts)
    part_width = model // count
    block = min(512, part_width)
    steps = part_width // block

    def column(h, j, place_ref):
        return (0, lax.rem(place_ref[0] - h + count, count) * steps + j)

    def part_at(part):
        return lambda h, j, _: (
            0,
            0,
            jnp.where(h == part, j, jnp.where(h < part, 0, steps - 1)),
        )

    def kernel(place_ref, *refs):
        project_kernel(place_ref, groups, *refs)

    return pl.pallas_call(
        kernel,
        grid_spec=pltpu.PrefetchScalarGridSpec(
            num_scalar_prefetch=1,
            grid=(count, steps),
            in_specs=[pl.BlockSpec((rows, width), lambda h, j, _: (0, 0))] * groups
            + [pl.BlockSpec((width, block), column)]
            + [pl.BlockSpec((groups - 1, width, block), part_at(p)) for p in range(count)]
            + [pl.BlockSpec((rows, block), column), pl.BlockSpec((1, block), column)],
            out_specs=pl.BlockSpec((rows, block), column),
        ),
        out_shape=jax.ShapeDtypeStruct(tokens.shape, BF16),
        name="project",
    )(place, *attended, own_weight, *parts, tokens, gate)


def ring(block, axis, count, step):
    return [
        lax.ppermute(block, axis, [((j + k * step) % count, j) for j in range(count)])
        for k in range(1, count)
    ]


def spread(block, axes, count):
    copies = jnp.broadcast_to(block[None], (count,) + block.shape)
    return lax.all_to_all(copies, axes, 0, 0)


def local(
    n_sp,
    n_tp,
    n_dp,
    latent_tokens,
    condition,
    shift_weight,
    scale_weight,
    gate_weight,
    norm_gain,
    query_down,
    query_gain,
    kv_down,
    kv_gain,
    rope_down,
    query_up,
    key_up,
    value_up,
    query_norm_gain,
    key_norm_gain,
    out_weight,
    context_latent,
    context_rope,
    context_lift,
):
    model = latent_tokens.shape[1]
    part_width = model // n_dp
    place = lax.axis_index("dp")
    with jax.named_scope("weight_ring"):
        own_part = lax.dynamic_slice_in_dim(out_weight, place * part_width, part_width, 1)
        others = jnp.stack(ring(own_part, "tp", n_tp, 1))
    with jax.named_scope("weight_swap"):
        weight_parts = [others] + ring(others, "dp", n_dp, -1)
    activated = jax.nn.silu(condition.astype(F32)).astype(BF16)[None]
    terms = jnp.concatenate(
        [
            jnp.dot(activated, weight, preferred_element_type=F32)
            for weight in (shift_weight, scale_weight, gate_weight)
        ],
        axis=0,
    )
    summed = jnp.sum(spread(terms, "sp", n_sp), axis=0)
    context_own = jnp.concatenate([context_latent, context_rope], axis=1).T
    context_own, summed = lax.optimization_barrier((context_own, summed))
    with jax.named_scope("context_ring"):
        context = jnp.stack([context_own] + ring(context_own, "sp", n_sp, 1))
    mod = jnp.transpose(spread(summed, "tp", n_tp), (1, 0, 2)).reshape(3, model)
    token_values = latent_tokens.astype(F32)
    normed = (rms_scaled(token_values, norm_gain) * (1.0 + mod[1]) + mod[0]).astype(BF16)
    key_latent = rms_scaled(
        jnp.dot(normed, kv_down, preferred_element_type=F32), kv_gain
    ).astype(BF16)
    rope_key = jnp.dot(normed, rope_down, preferred_element_type=F32).astype(BF16)
    query_latent = rms_scaled(
        jnp.dot(normed, query_down, preferred_element_type=F32), query_gain
    ).astype(BF16)
    with jax.named_scope("query_ring"):
        query_group = jnp.concatenate([query_latent] + ring(query_latent, "tp", n_tp, 1), axis=0)
    column = spread(jnp.concatenate([key_latent, rope_key], axis=1).T, "sp", n_sp)
    latent = spread(column, "tp", n_tp)
    latent = latent.reshape((n_tp * n_sp,) + latent.shape[2:])
    block_rows = query_latent.shape[0]
    group_rows = query_group.shape[0]
    tables = turn_tables(n_sp * group_rows)
    starts = lax.axis_index("sp") * group_rows + block_rows * (
        (lax.axis_index("tp") + jnp.arange(n_tp)) % n_tp
    )
    own = [
        jnp.concatenate(
            [
                lax.dynamic_slice_in_dim(jnp.asarray(t), starts[k], block_rows, 1)
                for k in range(n_tp)
            ],
            axis=1,
        )
        for t in tables
    ]
    every = [
        jnp.asarray(
            t.reshape(-1, n_sp, n_tp, block_rows).transpose(0, 2, 1, 3).reshape(t.shape)
        )
        for t in tables
    ]
    attended = attend(
        query_group,
        latent,
        context,
        query_up,
        key_up,
        value_up,
        (query_norm_gain[:, None], key_norm_gain[:, None]),
        context_lift[None],
        (*own, *every),
    )
    blocks = [attended[k * block_rows : (k + 1) * block_rows] for k in range(n_tp)]
    with jax.named_scope("attended_ring"):
        shared = [blocks[0]] + [
            lax.ppermute(blocks[-k % n_tp], "tp", [((j + k) % n_tp, j) for j in range(n_tp)])
            for k in range(1, n_tp)
        ]
    return project(place[None], shared, out_weight, weight_parts, latent_tokens, mod[2:3])


def solution(mesh):
    in_specs = (
        P(("dp", "sp", "tp"), None),
        P(("dp", "sp")),
        P("sp", "tp"),
        P("sp", "tp"),
        P("sp", "tp"),
        P(),
        P(),
        P(),
        P(),
        P(),
        P(),
        P(None, "tp"),
        P(None, "tp"),
        P(None, "tp"),
        P(),
        P(),
        P("tp", None),
        P(("dp", "sp"), None),
        P(("dp", "sp"), None),
        P("tp"),
    )
    out_specs = P(("dp", "sp", "tp"), None)
    body = functools.partial(local, mesh.shape["sp"], mesh.shape["tp"], mesh.shape["dp"])
    return jax.shard_map(body, mesh=mesh, in_specs=in_specs, out_specs=out_specs, check_vma=False)
```

```python
import functools
import math

import jax
import jax.numpy as jnp
import numpy as np
from jax import lax
from jax.experimental import pallas as pl
from jax.experimental.pallas import tpu as pltpu
from jax.sharding import PartitionSpec as P

NOPE_DIM = 64
ROPE_DIM = 32
VALUE_DIM = 64
QK_DIM = 96
PAD_DIM = 128
GRID_W = 64

EPS = 1e-06
THETA = 10000.0


F32 = jnp.float32
BF16 = jnp.bfloat16


def rms_scaled(values, gain_vector):
    mean_square = jnp.mean(values * values, axis=-1, keepdims=True)
    return values * lax.rsqrt(mean_square + EPS) * gain_vector


def turn_tables(token_count):
    freq_count = ROPE_DIM // 4
    inverse = (THETA ** (-4.0 * np.arange(freq_count) / ROPE_DIM)).astype(np.float32)
    index = np.arange(token_count)
    row = (index // GRID_W).astype(np.float32)
    col = (index % GRID_W).astype(np.float32)
    angles = np.concatenate([inverse[:, None] * row, inverse[:, None] * col], axis=0)
    angles = angles.astype(np.float64)
    return np.cos(angles).astype(np.float32), np.sin(angles).astype(np.float32)


def turn(part, cosine, sine):
    f = ROPE_DIM // 4
    u0, w0, u1, w1 = part[:f], part[f : 2 * f], part[2 * f : 3 * f], part[3 * f :]
    c0, c1, s0, s1 = cosine[:f], cosine[f:], sine[:f], sine[f:]
    return jnp.concatenate(
        [u0 * c0 - w0 * s0, w0 * c0 + u0 * s0, u1 * c1 - w1 * s1, w1 * c1 + u1 * s1], axis=0
    )


def contract(a, b, dims):
    return lax.dot_general(a, b, (dims, ((), ())), preferred_element_type=F32)


def attention_kernel(
    *refs,
    query_blocks,
    context_blocks,
    head_count,
    chunk,
    row_block,
):
    query_refs, refs = refs[:query_blocks], refs[query_blocks:]
    context_refs, refs = refs[:context_blocks], refs[context_blocks:]
    (
        latent_ref,
        query_up_ref,
        key_up_ref,
        value_up_ref,
        query_gain_ref,
        key_gain_ref,
        lift_ref,
        starts_ref,
        cos_ref,
        sin_ref,
    ) = refs[:10]
    out_refs = refs[10 : 10 + query_blocks]
    keys, values, queries, scores = refs[10 + query_blocks :]
    rank = key_up_ref.shape[0]
    latent_block = latent_ref.shape[2]
    context_block = context_refs[0].shape[1]
    latent_count = latent_ref.shape[0] * latent_block
    context_count = context_blocks * context_block
    key_count = latent_count + context_count
    query_block = query_refs[0].shape[0]
    row_count = query_blocks * query_block
    diagonal = lax.broadcasted_iota(jnp.int32, (QK_DIM, QK_DIM), 0) == lax.broadcasted_iota(
        jnp.int32, (QK_DIM, QK_DIM), 1
    )
    key_gain = jnp.sum(jnp.where(diagonal, key_gain_ref[...], 0.0), axis=1, keepdims=True)
    query_gain = jnp.sum(jnp.where(diagonal, query_gain_ref[...], 0.0), axis=1, keepdims=True)
    def build(rows, target, width, tables, is_context):
        latent = rows[:rank]
        nope = contract(key_up_ref[...], latent, ((0,), (0,)))
        rope = rows[rank : rank + ROPE_DIM].astype(F32)
        rope_square = jnp.sum(rope * rope, axis=0, keepdims=True)
        rope = rope * key_gain[NOPE_DIM:]
        if tables is not None:
            rope = turn(rope, *tables)
        for head in range(head_count):
            part = nope[head * NOPE_DIM : (head + 1) * NOPE_DIM]
            square = jnp.sum(part * part, axis=0, keepdims=True) + rope_square
            inverse = lax.rsqrt(square * (1.0 / QK_DIM) + EPS)
            if is_context:
                lift = jnp.full((16, width), lift_ref[0, head] * math.sqrt(QK_DIM), F32)
                high = lift.astype(BF16).astype(F32)
                middle = (lift - high).astype(BF16).astype(F32)
                low = lift - high - middle
                index = lax.broadcasted_iota(jnp.int32, (16, width), 0)
                extra = jnp.where(
                    index == 0,
                    high,
                    jnp.where(index == 1, middle, jnp.where(index == 2, low, 0.0)),
                )
            else:
                extra = jnp.zeros((16, width), F32)
            keys[head, :, target] = jnp.concatenate(
                [
                    part * key_gain[:NOPE_DIM] * inverse,
                    rope * inverse,
                    extra,
                    jnp.zeros((16, width), F32),
                ],
                axis=0,
            ).astype(BF16)
        value = contract(latent, value_up_ref[...], ((0,), (0,)))
        lane = lax.broadcasted_iota(jnp.int32, (width, PAD_DIM), 1)
        for pair in range(head_count // 2):
            both = value[:, pair * PAD_DIM : (pair + 1) * PAD_DIM]
            one_even = (lane == VALUE_DIM).astype(F32)
            one_odd = (lane == 0).astype(F32)
            values[2 * pair, target, :] = jnp.where(lane < VALUE_DIM, both, one_even).astype(BF16)
            values[2 * pair + 1, target, :] = jnp.where(
                lane >= VALUE_DIM, both, one_odd
            ).astype(BF16)

    def latent_chunk(i, carry):
        at = pl.ds(pl.multiple_of(i * chunk, chunk), chunk)
        count = chunk // latent_block
        rows = jnp.concatenate([latent_ref[i * count + j] for j in range(count)], axis=1)
        build(rows, at, chunk, (cos_ref[:, at], sin_ref[:, at]), False)
        return carry

    lax.fori_loop(0, latent_count // chunk, latent_chunk, 0)

    context_step = chunk // context_block
    for i in range(context_count // chunk):
        part = context_refs[i * context_step : (i + 1) * context_step]
        rows = jnp.concatenate([ref[...] for ref in part], axis=1)
        first = latent_count + i * chunk
        build(rows, slice(first, first + chunk), chunk, None, True)

    query_rows = jnp.concatenate([ref[...] for ref in query_refs], axis=0)

    def own_table(ref):
        return jnp.concatenate(
            [
                ref[:, pl.ds(pl.multiple_of(starts_ref[k], query_block), query_block)]
                for k in range(query_blocks)
            ],
            axis=1,
        )

    own_cos, own_sin = own_table(cos_ref), own_table(sin_ref)
    projected = contract(query_up_ref[...], query_rows, ((0,), (1,)))
    for head in range(head_count):
        part = projected[head * QK_DIM : (head + 1) * QK_DIM]
        inverse = lax.rsqrt(jnp.mean(part * part, axis=0, keepdims=True) + EPS)
        part = part * inverse * query_gain
        turned = turn(part[NOPE_DIM:], own_cos, own_sin)
        extra = (
            lax.broadcasted_iota(jnp.int32, (PAD_DIM - QK_DIM, row_count), 0) < 3
        ).astype(F32)
        whole = jnp.concatenate([part[:NOPE_DIM], turned, extra], axis=0)
        queries[head] = whole.T.astype(BF16)

    scale = QK_DIM**-0.5 * math.log2(math.e)
    chunks = key_count // chunk
    blocks = row_count // row_block

    def score_chunk(slot, head, rows, index, top):
        at = slice(index * chunk, (index + 1) * chunk)
        part = jnp.dot(queries[head, rows, :], keys[head, :, at], preferred_element_type=F32)
        scores[slot, :, at] = part
        for start in range(0, chunk, PAD_DIM):
            piece = part[:, start : start + PAD_DIM]
            top = piece if top is None else jnp.maximum(top, piece)
        return top

    def weigh_chunk(slot, head, index, top, total):
        at = slice(index * chunk, (index + 1) * chunk)
        weights = jnp.exp2((scores[slot, :, at] - top) * scale).astype(BF16)
        product = jnp.dot(weights, values[head, at, :], preferred_element_type=F32)
        return product if total is None else total + product

    def both_steps(slot, head, top, next_head, next_rows):
        top = jnp.max(top, axis=1, keepdims=True)
        next_top = None
        total = None
        for index in range(chunks):
            next_top = score_chunk(1 - slot, next_head, next_rows, index, next_top)
            total = weigh_chunk(slot, head, index, top, total)
        return total, next_top

    first = None
    for index in range(chunks):
        first = score_chunk(0, 0, slice(0, row_block), index, first)

    lane = lax.broadcasted_iota(jnp.int32, (row_block, PAD_DIM), 1)

    def pair_step(pair, top):
        even, odd = 2 * pair, 2 * pair + 1
        following = jnp.minimum(even + 2, head_count - 2)
        for block in range(blocks):
            rows = slice(block * row_block, (block + 1) * row_block)
            even_total, top = both_steps(0, even, top, odd, rows)
            if block + 1 < blocks:
                next_head = even
                next_rows = slice((block + 1) * row_block, (block + 2) * row_block)
            else:
                next_head = following
                next_rows = slice(0, row_block)
            odd_total, top = both_steps(1, odd, top, next_head, next_rows)
            joined = jnp.where(
                lane < VALUE_DIM,
                even_total / even_total[:, VALUE_DIM : VALUE_DIM + 1],
                odd_total / odd_total[:, 0:1],
            )
            joined = joined.astype(BF16)
            columns = pl.ds(pl.multiple_of(pair * PAD_DIM, PAD_DIM), PAD_DIM)
            for piece in range(row_block // query_block):
                out_refs[block * (row_block // query_block) + piece][:, columns] = joined[
                    piece * query_block : (piece + 1) * query_block
                ]
        return top

    lax.fori_loop(0, head_count // 2, pair_step, first)


def attend(query, context, latent, query_up, key_up, value_up, gains, lift, starts, tables):
    block_rows = query[0].shape[0]
    row_count = len(query) * block_rows
    key_count = latent.shape[0] * latent.shape[2] + len(context) * context[0].shape[1]
    head_count = query_up.shape[1] // QK_DIM
    vmem = pl.BlockSpec(memory_space=pltpu.VMEM)
    smem = pl.BlockSpec(memory_space=pltpu.SMEM)
    one_out = jax.ShapeDtypeStruct((block_rows, head_count * VALUE_DIM), BF16)
    row_block = min(256, row_count)
    return pl.pallas_call(
        functools.partial(
            attention_kernel,
            query_blocks=len(query),
            context_blocks=len(context),
            head_count=head_count,
            chunk=512,
            row_block=row_block,
        ),
        out_shape=[one_out] * len(query),
        in_specs=[vmem] * (len(query) + len(context) + 6) + [smem] * 2 + [vmem] * 2,
        out_specs=[vmem] * len(query),
        scratch_shapes=[
            pltpu.VMEM((head_count, PAD_DIM, key_count), BF16),
            pltpu.VMEM((head_count, key_count, PAD_DIM), BF16),
            pltpu.VMEM((head_count, row_count, PAD_DIM), BF16),
            pltpu.VMEM((2, row_block, key_count), F32),
        ],
        compiler_params=pltpu.CompilerParams(vmem_limit_bytes=60 * 1024 * 1024),
        name="attend",
    )(*query, *context, latent, query_up, key_up, value_up, *gains, lift, starts, *tables)


def project_kernel(place_ref, groups, *refs):
    attended, own_ref = refs[:groups], refs[groups]
    token_ref, gate_ref, out_ref = refs[-3:]
    weight_refs = refs[groups + 1 : -3]
    for part in range(len(weight_refs) // (groups - 1)):
        part_refs = weight_refs[part * (groups - 1) : (part + 1) * (groups - 1)]

        @pl.when(pl.program_id(0) == part)
        def _():
            mixed = None
            for group in range(groups):
                weight = own_ref[...] if group == 0 else part_refs[group - 1][...]
                term = jnp.dot(attended[group][...], weight, preferred_element_type=F32)
                term = term.astype(BF16).astype(F32)
                mixed = term if mixed is None else mixed + term
            out_ref[...] = (token_ref[...].astype(F32) + gate_ref[...] * mixed).astype(BF16)


def project(place, attended, own_weight, parts, tokens, gate):
    groups = len(attended)
    rows, width = attended[0].shape
    model = tokens.shape[1]
    count = len(parts)
    part_width = model // count
    block = min(512, part_width)
    steps = part_width // block

    def column(h, j, place_ref):
        return (0, lax.rem(place_ref[0] - h + count, count) * steps + j)

    def part_at(part):
        return lambda h, j, _: (
            0,
            jnp.where(h == part, j, jnp.where(h < part, 0, steps - 1)),
        )

    def kernel(place_ref, *refs):
        project_kernel(place_ref, groups, *refs)

    return pl.pallas_call(
        kernel,
        grid_spec=pltpu.PrefetchScalarGridSpec(
            num_scalar_prefetch=1,
            grid=(count, steps),
            in_specs=[pl.BlockSpec((rows, width), lambda h, j, _: (0, 0))] * groups
            + [pl.BlockSpec((width, block), column)]
            + [
                pl.BlockSpec((width, block), part_at(p))
                for p in range(count)
                for _ in range(groups - 1)
            ]
            + [pl.BlockSpec((rows, block), column), pl.BlockSpec((1, block), column)],
            out_specs=pl.BlockSpec((rows, block), column),
        ),
        out_shape=jax.ShapeDtypeStruct(tokens.shape, BF16),
        name="project",
    )(place, *attended, own_weight, *sum(parts, []), tokens, gate)


def ring(block, axis, count, step):
    return [
        lax.ppermute(block, axis, [((j + k * step) % count, j) for j in range(count)])
        for k in range(1, count)
    ]


def spread(block, axes, count):
    copies = jnp.broadcast_to(block[None], (count,) + block.shape)
    return lax.all_to_all(copies, axes, 0, 0)


def local(
    n_sp,
    n_tp,
    n_dp,
    latent_tokens,
    condition,
    shift_weight,
    scale_weight,
    gate_weight,
    norm_gain,
    query_down,
    query_gain,
    kv_down,
    kv_gain,
    rope_down,
    query_up,
    key_up,
    value_up,
    query_norm_gain,
    key_norm_gain,
    out_weight,
    context_latent,
    context_rope,
    context_lift,
):
    model = latent_tokens.shape[1]
    part_width = model // n_dp
    place = lax.axis_index("dp")
    activated = jax.nn.silu(condition.astype(F32)).astype(BF16)[None]
    terms = jnp.concatenate(
        [
            jnp.dot(activated, weight, preferred_element_type=F32)
            for weight in (shift_weight, scale_weight, gate_weight)
        ],
        axis=0,
    )
    summed = jnp.sum(spread(terms, "sp", n_sp), axis=0)
    context_own = jnp.concatenate([context_latent, context_rope], axis=1).T
    own_part = lax.dynamic_slice_in_dim(out_weight, place * part_width, part_width, 1)
    context_own, own_part, summed = lax.optimization_barrier((context_own, own_part, summed))
    with jax.named_scope("weight_ring"):
        others = ring(own_part, "tp", n_tp, 1)
    with jax.named_scope("context_ring"):
        context = [context_own] + ring(context_own, "sp", n_sp, 1)
    mod = jnp.transpose(spread(summed, "tp", n_tp), (1, 0, 2)).reshape(3, model)
    token_values = latent_tokens.astype(F32)
    normed = (rms_scaled(token_values, norm_gain) * (1.0 + mod[1]) + mod[0]).astype(BF16)
    key_latent = rms_scaled(
        jnp.dot(normed, kv_down, preferred_element_type=F32), kv_gain
    ).astype(BF16)
    rope_key = jnp.dot(normed, rope_down, preferred_element_type=F32).astype(BF16)
    query_latent = rms_scaled(
        jnp.dot(normed, query_down, preferred_element_type=F32), query_gain
    ).astype(BF16)
    with jax.named_scope("query_ring"):
        query_blocks = ring(query_latent, "tp", n_tp, 1)
    column = spread(jnp.concatenate([key_latent, rope_key], axis=1).T, "sp", n_sp)
    column, query_blocks = lax.optimization_barrier((column, query_blocks))
    latent = spread(column, "tp", n_tp)
    others, _ = lax.optimization_barrier((others, latent))
    latent = latent.reshape((n_tp * n_sp,) + latent.shape[2:])
    with jax.named_scope("weight_swap"):
        swaps = [ring(other, "dp", n_dp, -1) for other in others]
    weight_parts = [others] + [[swap[d] for swap in swaps] for d in range(n_dp - 1)]
    block_rows = query_latent.shape[0]
    group_rows = n_tp * block_rows
    tables = [
        jnp.asarray(t.reshape(-1, n_sp, n_tp, block_rows).transpose(0, 2, 1, 3).reshape(t.shape))
        for t in turn_tables(n_sp * group_rows)
    ]
    starts = block_rows * (
        ((lax.axis_index("tp") + jnp.arange(n_tp, dtype=jnp.int32)) % n_tp) * n_sp
        + lax.axis_index("sp")
    )
    blocks = attend(
        [query_latent] + query_blocks,
        context,
        latent,
        query_up,
        key_up,
        value_up,
        (query_norm_gain[None], key_norm_gain[None]),
        context_lift[None],
        starts,
        tables,
    )
    with jax.named_scope("attended_ring"):
        shared = [blocks[0]] + [
            lax.ppermute(blocks[-k % n_tp], "tp", [((j + k) % n_tp, j) for j in range(n_tp)])
            for k in range(1, n_tp)
        ]
    return project(place[None], shared, out_weight, weight_parts, latent_tokens, mod[2:3])


def solution(mesh):
    in_specs = (
        P(("dp", "sp", "tp"), None),
        P(("dp", "sp")),
        P("sp", "tp"),
        P("sp", "tp"),
        P("sp", "tp"),
        P(),
        P(),
        P(),
        P(),
        P(),
        P(),
        P(None, "tp"),
        P(None, "tp"),
        P(None, "tp"),
        P(),
        P(),
        P("tp", None),
        P(("dp", "sp"), None),
        P(("dp", "sp"), None),
        P("tp"),
    )
    out_specs = P(("dp", "sp", "tp"), None)
    body = functools.partial(local, mesh.shape["sp"], mesh.shape["tp"], mesh.shape["dp"])
    return jax.shard_map(body, mesh=mesh, in_specs=in_specs, out_specs=out_specs, check_vma=False)
```
